32 devices in a mesh: ep: 4 (over z), tp: 8 (over y, x, core).
Axes of the slice: x: 2, y: 2, z: 4, core: 2. Of those that a mesh axis runs over, the one named last changes fastest.
Arguments:
- tokens: bfloat16 [1024, 2048], P('ep'), may hold values from -6 to 6
- norm_gain: float32 [2048], replicated, may hold values from 0.1 to 1.9
- expert_ids: int32 [1024, 2], P('ep'), may hold values from 0 to 3, all different within a row; in each aligned block of 256 rows (0 to 255, 256 to 511, ...) at most 192 rows name the same one
- routing_weight: float32 [1024, 2], P('ep'), may hold values from 0.1 to 1
- expert_gate: bfloat16 [4, 2048, 5632], P('ep', None, 'tp'), may hold values from -0.125 to 0.125
- expert_up: bfloat16 [4, 2048, 5632], P('ep', None, 'tp'), may hold values from -0.125 to 0.125
- expert_down: bfloat16 [4, 5632, 2048], P('ep', 'tp'), may hold values from -0.078125 to 0.078125
- dense_gate_w: bfloat16 [2048, 1024], P(None, 'tp'), may hold values from -0.125 to 0.125
- dense_up_w: bfloat16 [2048, 1024], P(None, 'tp'), may hold values from -0.125 to 0.125
- dense_down_w: bfloat16 [1024, 2048], P('tp'), may hold values from -0.1875 to 0.1875
- dense_gate: float32 [2048], P('tp'), may hold values from -3 to 3
Outputs:
- layer_out: bfloat16 [1024, 2048], P('ep', 'tp')
The draws below stay inside these ranges and needn't reach their ends.
Inputs may be any that keep to these rules, and one draw needn't show every extreme that they name: `expert_ids`: within the 256 rows of one device along ep, each row names two different experts and no expert is named by more than 192 rows; some expert is named by exactly 192 rows.
All inputs are finite; a program needn't handle non-finite values.
Results may differ from the reference program's by a relative error of at most 0.017.
Values may be sent and summed in bfloat16 or wider, within the bound.
A program may use at most 64 MiB of HBM per device.

```python
import math
import jax
import jax.numpy as jnp
import numpy as np
from jax import lax

D = 2048
FF = 5632
DS = 1024
TOK_G = 256
EXPERTS = 4
CAP = 192
TOKENS = 1024
FF_PART = 704
DS_PART = 128
N_EP = 4
N_TP = 8


def block_levels(stream_key, dims, cuts, least, high):
    loudness, own = 1.0, jax.random.fold_in(stream_key, 6)
    for position, parts in cuts:
        steps = jnp.exp(jax.random.uniform(jax.random.fold_in(own, position), (parts,), jnp.float32, least / len(cuts), high / len(cuts)))
        loudness = loudness * jnp.repeat(steps, dims[position] // parts).reshape([-1 if axis == position else 1 for axis in range(len(dims))])
    return loudness


def shared_out(stream_key, own, number, rows, number_of, top, most, slope):
    order = jax.random.permutation(stream_key, number_of)
    packed, usual = portions_of(number_of, rows * top, most, slope, True), portions_of(number_of, rows * top, most, slope, False)
    places = jnp.arange(number_of)

    def named(lengths, offset_by):
        used = int((lengths > 0).sum())
        fixed = max(1, used // 4)
        shifted = fixed + (places - fixed + offset_by * (used - fixed)) % max(1, number_of - fixed)
        return jnp.zeros((number_of,), jnp.int32).at[order[jnp.where(places < fixed, places, shifted)]].set(jnp.asarray(lengths, jnp.int32))

    lengths = jnp.where(number % 4 == 0, named(packed, number // 4), named(usual, number - number // 4 - 1))
    mixed = jax.random.permutation(jax.random.fold_in(own, 3), number_of)
    donor, receiver = mixed[0:number_of // 2 * 2:2], mixed[1:number_of // 2 * 2:2]
    margin = jnp.minimum(lengths[donor] - 1, most - lengths[receiver]) // 2
    margin = jnp.where((donor == order[0]) | (receiver == order[0]) | (lengths[receiver] == 0), 0, jnp.maximum(margin, 0))
    shifted = jax.random.randint(jax.random.fold_in(own, 4), (number_of // 2,), 0, 1 << 20) % (margin + 1)
    lengths = lengths.at[donor].add(-shifted).at[receiver].add(shifted)
    labels = jnp.searchsorted(jnp.cumsum(lengths), jnp.arange(rows * top), side="right").astype(jnp.int32)
    table = labels.reshape(top, rows).T
    table = table[jax.random.permutation(jax.random.fold_in(own, 1), rows)]
    offset_by = jax.random.randint(jax.random.fold_in(own, 2), (rows, 1), 0, top)
    return jnp.take_along_axis(table, (jnp.arange(top)[None, :] + offset_by) % top, axis=1)


def portions_of(number_of, total, reach, skew, full):
    weights = [(1 << 20) // math.isqrt(standing ** skew) + 1 for standing in range(1, number_of + 1)]
    largest = reach if full else min(reach, max(-(-total // number_of), total * weights[0] // sum(weights)))
    least = 1 if total - largest >= number_of - 1 else 0
    given, rest = [largest] + [least] * (number_of - 1), total - largest - least * (number_of - 1)
    while rest > 0:
        free = [i for i in range(1, number_of) if given[i] < largest] or [i for i in range(1, number_of) if given[i] < reach]
        pool, remaining = sum([weights[i] for i in free]), rest
        for i in free:
            extra = min(reach - given[i], max(1, remaining * weights[i] // pool), rest)
            given[i] = given[i] + extra
            rest = rest - extra
    return np.array(given)


def noise(stream_key, dims, scale, reach, split=(), kind=jnp.bfloat16):
    values = scale * jax.random.normal(stream_key, dims, jnp.float32)
    if split:
        values = values * block_levels(stream_key, dims, split, -0.22, 0.18)
    return jnp.clip(values, -reach, reach).astype(kind)


def setup_inputs(seed: int = 0) -> dict:
    splits = jax.random.split(jax.random.key(seed), 12)
    tokens = noise(splits[0], (TOKENS, D), 1.0, 6.0, ((0, 4),))
    norm_gain = jnp.clip(1.0 + 0.18 * jax.random.normal(splits[1], (D,), jnp.float32), 0.1, 1.9)
    expert_ids_keys = jax.random.split(jax.random.fold_in(splits[2], 1), TOKENS // TOK_G)
    expert_ids_turns = jax.random.permutation(jax.random.fold_in(splits[2], 3), TOKENS // TOK_G)
    expert_ids = jax.vmap(lambda own, number: shared_out(jax.random.fold_in(splits[2], 2), own, number, TOK_G, EXPERTS, 2, CAP, 2))(expert_ids_keys, expert_ids_turns).reshape((TOKENS, 2))
    routing_weight = jnp.clip(0.1 + 0.9 * jax.random.uniform(splits[3], (TOKENS, 2), jnp.float32) ** block_levels(splits[3], (TOKENS, 2), ((0, 4),), -0.2, 0.2), 0.1, 1.0)
    expert_gate = noise(splits[4], (EXPERTS, D, FF), D ** -0.5, 0.125, ((0, 4), (2, 8)))
    expert_up = noise(splits[5], (EXPERTS, D, FF), D ** -0.5, 0.125, ((0, 4), (2, 8)))
    expert_down = noise(splits[6], (EXPERTS, FF, D), FF ** -0.5, 0.078125, ((0, 4), (1, 8)))
    dense_gate_w = noise(splits[7], (D, DS), D ** -0.5, 0.125, ((1, 8),))
    dense_up_w = noise(splits[8], (D, DS), D ** -0.5, 0.125, ((1, 8),))
    dense_down_w = noise(splits[9], (DS, D), DS ** -0.5, 0.1875, ((0, 8),))
    dense_gate = jnp.clip(jax.random.uniform(splits[10], (D,), jnp.float32, -3.0, 3.0) * block_levels(splits[10], (D,), ((0, 8),), -0.4, 0.0), -3.0, 3.0)
    return {"tokens": tokens, "norm_gain": norm_gain, "expert_ids": expert_ids, "routing_weight": routing_weight, "expert_gate": expert_gate, "expert_up": expert_up, "expert_down": expert_down, "dense_gate_w": dense_gate_w, "dense_up_w": dense_up_w, "dense_down_w": dense_down_w, "dense_gate": dense_gate}


EPSILON = 1e-06

def normalize(tokens, norm_gain):
    values = tokens.astype(jnp.float32)
    factor = lax.rsqrt(lax.optimization_barrier(jnp.mean(values * values, axis=-1, keepdims=True)) + EPSILON)
    return (values * factor * norm_gain[None, :]).astype(jnp.bfloat16)

def positions(block_ids):
    flat_ids = block_ids.reshape(-1)
    one_hot = (flat_ids[:, None] == jnp.arange(EXPERTS, dtype=jnp.int32)[None, :]).astype(jnp.int32)
    earlier = jnp.cumsum(one_hot, axis=0) - one_hot
    return flat_ids * CAP + lax.optimization_barrier(jnp.sum(earlier * one_hot, axis=1))

def fill_table(place_row):
    token_no = jnp.arange(2 * TOK_G, dtype=jnp.int32) // 2 + 1
    return jnp.zeros((EXPERTS * CAP,), jnp.int32).at[place_row].set(token_no)

def pick_rows(table, index_row):
    return table[index_row]

def block_sum(hidden, down_w, part_size):
    row_count = hidden.shape[0]
    pieces = hidden.reshape(row_count, N_TP, part_size).astype(jnp.float32)
    weights = down_w.reshape(N_TP, part_size, down_w.shape[1]).astype(jnp.float32)
    partial_value = jnp.einsum('rpf,pfd->rpd', pieces, weights).astype(jnp.bfloat16)
    partial_value = lax.optimization_barrier(partial_value)
    return lax.optimization_barrier(jnp.sum(partial_value.astype(jnp.float32), axis=1))

def reference(tokens, norm_gain, expert_ids, routing_weight, expert_gate, expert_up, expert_down, dense_gate_w, dense_up_w, dense_down_w, dense_gate):
    normed = normalize(tokens, norm_gain)
    normed_blocks = normed.reshape(N_EP, TOK_G, D)
    places = jax.vmap(positions)(expert_ids.reshape(N_EP, TOK_G, 2))
    sources = jax.vmap(fill_table)(places)
    padded = jnp.concatenate([jnp.zeros((N_EP, 1, D), jnp.bfloat16), normed_blocks], axis=1)
    gathered = jax.vmap(pick_rows)(padded, sources)
    expert_rows = gathered.reshape(N_EP, EXPERTS, CAP, D).transpose(1, 0, 2, 3).reshape(EXPERTS, N_EP * CAP, D)

    def one_expert(operands):
        rows_in, gate_w, up_w, down_w = operands
        gate_act = jnp.dot(rows_in, gate_w, preferred_element_type=jnp.float32)
        up_act = jnp.dot(rows_in, up_w, preferred_element_type=jnp.float32)
        hidden = (jax.nn.silu(gate_act) * up_act).astype(jnp.bfloat16)
        return block_sum(hidden, down_w, FF_PART)
    expert_out = lax.map(one_expert, (expert_rows, expert_gate, expert_up, expert_down)).astype(jnp.bfloat16)
    by_source = expert_out.reshape(EXPERTS, N_EP, CAP, D).transpose(1, 0, 2, 3).reshape(N_EP, EXPERTS * CAP, D)
    picked = jax.vmap(pick_rows)(by_source, places).reshape(TOKENS, 2, D).astype(jnp.float32)
    routed = lax.optimization_barrier(jnp.sum(routing_weight[:, :, None] * picked, axis=1))

    def dense_block(block_rows):
        gate_act = jnp.dot(block_rows, dense_gate_w, preferred_element_type=jnp.float32)
        up_act = jnp.dot(block_rows, dense_up_w, preferred_element_type=jnp.float32)
        hidden = (jax.nn.silu(gate_act) * up_act).astype(jnp.bfloat16)
        return block_sum(hidden, dense_down_w, DS_PART)
    dense_out = lax.map(dense_block, normed_blocks).reshape(TOKENS, D)
    layer_out = routed + jax.nn.sigmoid(dense_gate)[None, :] * dense_out
    return layer_out.astype(jnp.bfloat16)
```

```python
import functools
import jax
import jax.numpy as jnp
from jax import lax
from jax.experimental import pallas as pl
from jax.experimental.pallas import tpu as pltpu
from jax.sharding import PartitionSpec as P

EPSILON = 1e-06


def positions(block_ids, experts, capacity):
    flat_ids = block_ids.reshape(-1)
    one_hot = (flat_ids[:, None] == jnp.arange(experts, dtype=jnp.int32)[None, :]).astype(jnp.int32)
    earlier = jnp.cumsum(one_hot, axis=0) - one_hot
    return flat_ids * capacity + jnp.sum(earlier * one_hot, axis=1)


def transposed_term(hidden, down_w):
    return lax.dot_general(
        down_w, hidden, (((0,), (1,)), ((), ())), preferred_element_type=jnp.float32
    )


def plain_local(
    tokens,
    norm_gain,
    expert_ids,
    routing_weight,
    expert_gate,
    expert_up,
    expert_down,
    dense_gate_w,
    dense_up_w,
    dense_down_w,
    dense_gate,
):
    experts = lax.axis_size("ep")
    group_tokens, model_width = tokens.shape
    capacity = 3 * group_tokens // experts
    slots_all = experts * capacity
    part_rows = model_width // lax.axis_size("tp")
    values = tokens.astype(jnp.float32)
    factor = lax.rsqrt(jnp.mean(values * values, axis=-1, keepdims=True) + EPSILON)
    normed = (values * factor * norm_gain[None, :]).astype(jnp.bfloat16)
    places = positions(expert_ids, experts, capacity)
    token_no = jnp.arange(2 * group_tokens, dtype=jnp.int32) // 2 + 1
    sources = jnp.zeros((slots_all,), jnp.int32).at[places].set(token_no)
    padded = jnp.concatenate([jnp.zeros((1, model_width), jnp.bfloat16), normed], axis=0)
    gate_w = expert_gate[0]
    up_w = expert_up[0]
    down_w = expert_down[0]
    first_col = lax.axis_index("tp") * part_rows
    column_part = lax.dynamic_slice_in_dim(padded, first_col, part_rows, 1)
    outgoing = column_part[sources].reshape(experts, capacity, part_rows)
    landed = lax.all_to_all(outgoing, "ep", split_axis=0, concat_axis=0, tiled=True)
    portion = lax.all_gather(landed, "tp", axis=2, tiled=True)
    columns = portion.reshape(slots_all, portion.shape[2])
    gate_act = jnp.dot(columns, gate_w, preferred_element_type=jnp.float32)
    up_act = jnp.dot(columns, up_w, preferred_element_type=jnp.float32)
    hidden = (jax.nn.silu(gate_act) * up_act).astype(jnp.bfloat16)
    dense_gate_act = jnp.dot(normed, dense_gate_w, preferred_element_type=jnp.float32)
    dense_up_act = jnp.dot(normed, dense_up_w, preferred_element_type=jnp.float32)
    dense_hidden = (jax.nn.silu(dense_gate_act) * dense_up_act).astype(jnp.bfloat16)
    dense_out = lax.psum_scatter(
        transposed_term(dense_hidden, dense_down_w).astype(jnp.bfloat16),
        "tp",
        scatter_dimension=0,
        tiled=True,
    ).astype(jnp.float32)
    expert_out = lax.psum_scatter(
        transposed_term(hidden, down_w).astype(jnp.bfloat16), "tp", scatter_dimension=0, tiled=True
    )
    expert_half = expert_out.reshape(part_rows, experts, capacity)
    returned = lax.all_to_all(expert_half, "ep", split_axis=1, concat_axis=1, tiled=True).reshape(
        part_rows, slots_all
    )
    picked = (
        jnp.take(returned, places, axis=1).astype(jnp.float32).reshape(part_rows, group_tokens, 2)
    )
    routed = jnp.sum(picked * routing_weight[None, :, :], axis=2)
    gate_factor = jax.nn.sigmoid(dense_gate)[:, None]
    return (routed + gate_factor * dense_out).T.astype(jnp.bfloat16)


BF = jnp.bfloat16
F32 = jnp.float32


def silu_mul(gate_act, up_act):
    return (gate_act / (1.0 + jnp.exp(-gate_act)) * up_act).astype(BF)


def fused_kernel(
    experts,
    tok_ref,
    gain_ref,
    ids_ref,
    rw_ref,
    gw_hbm,
    uw_hbm,
    dw_hbm,
    dg_hbm,
    du_hbm,
    dd_hbm,
    dgate_ref,
    out_ref,
    gw,
    uw,
    dw,
    dgu,
    dd,
    normed,
    slot_row,
    slot_col,
    gates,
    zsend,
    xloc,
    xbuf,
    hid,
    dhid,
    part_l,
    part_c,
    r0_l,
    r0_c,
    r1a_l,
    r1b_l,
    r1a_c,
    r1b_c,
    r2a_l,
    r2b_l,
    r2a_c,
    r2b_c,
    fin,
    ret,
    total,
    wsem,
    gsem,
    zsem,
    agsem,
    rssem,
    retsem,
):
    me = lax.axis_index("ep")
    tp = lax.axis_index("tp")
    core, xx, yy = tp % 2, (tp // 2) % 2, tp // 4
    group, width = tok_ref.shape
    cols = out_ref.shape[1]
    cap = zsend.shape[1]
    ffp = gw.shape[1]
    dsp = dd.shape[0]
    rounds = experts - 1
    mesh_id = pl.DeviceIdType.MESH

    def peer(flip):
        bits = (core + flip % 2) % 2, (xx + flip // 2 % 2) % 2, (yy + flip // 4) % 2
        return bits[2] * 4 + bits[1] * 2 + bits[0]

    def ring(d):
        return lax.rem(me + d, experts)

    barrier = pltpu.get_barrier_semaphore()
    for flip in range(1, 8):
        pl.semaphore_signal(barrier, 1, device_id=(me, peer(flip)), device_id_type=mesh_id)
    for d in range(1, experts):
        pl.semaphore_signal(barrier, 1, device_id=(ring(d), tp), device_id_type=mesh_id)

    loads = [
        pltpu.make_async_copy(gw_hbm.at[0], gw, wsem.at[0]),
        pltpu.make_async_copy(uw_hbm.at[0], uw, wsem.at[1]),
        pltpu.make_async_copy(dg_hbm, dgu.at[:, pl.ds(0, dsp)], wsem.at[2]),
        pltpu.make_async_copy(du_hbm, dgu.at[:, pl.ds(dsp, dsp)], wsem.at[3]),
        pltpu.make_async_copy(dw_hbm.at[0], dw, wsem.at[4]),
        pltpu.make_async_copy(dd_hbm, dd, wsem.at[5]),
    ]
    for load in loads:
        load.start()

    gain = gain_ref[...]
    step = 32

    def norm_rows(i, carry):
        rows = pl.ds(pl.multiple_of(i * step, step), step)
        values = tok_ref[rows, :].astype(F32)
        factor = lax.rsqrt(jnp.sum(values * values, axis=1, keepdims=True) * (1.0 / width) + EPSILON)
        normed[rows, :] = (values * factor * gain).astype(BF)
        return carry

    lax.fori_loop(0, group // step, norm_rows, 0)

    ids = ids_ref[...]
    id0, id1 = ids[:, 0:1], ids[:, 1:2]
    lane = lax.broadcasted_iota(jnp.int32, (group, 128), 1)
    named = (id0 == lane) | (id1 == lane)
    marks = jnp.where(named, 1.0, 0.0)
    earlier = jnp.where(
        lax.broadcasted_iota(jnp.int32, (group, group), 1)
        < lax.broadcasted_iota(jnp.int32, (group, group), 0),
        1.0,
        0.0,
    ).astype(BF)
    count = jnp.dot(earlier, marks.astype(BF), preferred_element_type=F32)
    slots = jnp.where(named, count, -1.0)
    slot_col[...] = slots
    slot_row[...] = slots.T

    def pick(e):
        row = slot_row[pl.ds(e, 1), :].astype(jnp.int32)
        where = lax.broadcasted_iota(jnp.int32, (cap, group), 0)
        return jnp.where(row == where, 1.0, 0.0).astype(BF)

    def combine(e):
        slot = jnp.sum(jnp.where(lane == e, slot_col[...], 0.0), axis=1, keepdims=True).astype(jnp.int32)
        rw = rw_ref[...]
        weight = jnp.where(id0 == e, rw[:, 0:1], 0.0) + jnp.where(id1 == e, rw[:, 1:2], 0.0)
        where = lax.broadcasted_iota(jnp.int32, (group, cap), 1)
        full = jnp.where(slot == where, weight, 0.0)
        high = full.astype(BF)
        return high, (full - high.astype(F32)).astype(BF)

    def mix(pair, rows):
        return jnp.dot(pair[0], rows, preferred_element_type=F32) + jnp.dot(
            pair[1], rows, preferred_element_type=F32
        )

    pl.semaphore_wait(barrier, 7 + rounds)

    pending = []

    def send(src, dst, sems, index, target):
        copy = pltpu.make_async_remote_copy(
            src_ref=src,
            dst_ref=dst,
            send_sem=sems.at[(0,) + index],
            recv_sem=sems.at[(1,) + index],
            device_id=target,
            device_id_type=mesh_id,
        )
        copy.start()
        pending.append(copy)
        return copy

    def at_tp(flip):
        return (me, peer(flip))

    def span(slice_no):
        return pl.ds(pl.multiple_of(slice_no * cols, cols), cols)

    zcopies, order = {}, list(range(1, experts))
    if rounds == 3:
        order = [1, 3, 2]
    for d in order:
        rows = jnp.dot(pick(ring(d)), normed[:, span(tp)], preferred_element_type=F32)
        zsend[d - 1] = rows.astype(BF)
        zcopies[d] = send(zsend.at[d - 1], xbuf.at[d - 1, :, span(tp)], zsem, (d - 1,), (ring(d), tp))
    gcopies = [send(dgate_ref, gates.at[tp], gsem, (f - 1,), at_tp(f)) for f in range(1, 8)]
    gates[tp] = dgate_ref[...]
    here = pick(me)

    def local_rows(k, carry):
        at = pl.ds(pl.multiple_of(k * cols, cols), cols)
        xloc[:, at] = jnp.dot(here, normed[:, at], preferred_element_type=F32).astype(BF)
        return carry

    lax.fori_loop(0, width // cols, local_rows, 0)

    half = cap // 2
    top, bottom = pl.ds(0, half), pl.ds(half, half)
    everything = pl.ds(0, cap)
    ag = {}

    def move(d, name, number, rows, slice_flip, flip):
        ref = xbuf.at[d - 1, rows, span(peer(slice_flip))]
        ag[d, name] = send(ref, ref, agsem, (d - 1, number), at_tp(flip))

    def ag1(d):
        zcopies[d].wait_recv()
        move(d, "x", 0, everything, 0, 2)
        move(d, "y", 1, everything, 0, 4)
        move(d, "c", 2, everything, 0, 1)

    def ag2(d):
        ag[d, "x"].wait_recv()
        move(d, "xy", 3, top, 2, 4)
        move(d, "xc", 4, everything, 2, 1)
        ag[d, "y"].wait_recv()
        move(d, "yx", 5, bottom, 4, 2)
        move(d, "yc", 6, everything, 4, 1)

    def ag3(d):
        ag[d, "xy"].wait_recv()
        move(d, "xyc", 7, top, 6, 1)
        ag[d, "yx"].wait_recv()
        move(d, "yxc", 8, bottom, 6, 1)

    def ag_done(d):
        for name in ("c", "xc", "yc", "xyc", "yxc"):
            ag[d, name].wait_recv()

    tiles = [(n, min(256, ffp - n)) for n in range(0, ffp, 256)]

    def hidden(rows_ref):
        for n, size in tiles:
            gate_act = jnp.dot(rows_ref[...], gw[:, n : n + size], preferred_element_type=F32)
            up_act = jnp.dot(rows_ref[...], uw[:, n : n + size], preferred_element_type=F32)
            hid[:, n : n + size] = silu_mul(gate_act, up_act)

    def rs_refs(b):
        if b == 0:
            return part_l, r0_l, r1a_l, r1b_l, r2a_l, r2b_l
        return tuple(r.at[b - 1] for r in (part_c, r0_c, r1a_c, r1b_c, r2a_c, r2b_c))

    rs = {}

    def rs0(b):
        part, r0 = rs_refs(b)[:2]
        rs[b, 0] = send(part.at[1 - core], r0, rssem, (b, 0), at_tp(1))

    def add(dst, index, other):
        dst[index] = (dst[index].astype(F32) + other.astype(F32)).astype(BF)

    def rs1(b):
        part, r0, r1a, r1b = rs_refs(b)[:4]
        h = part.shape[3] // 2
        rs[b, 0].wait_recv()
        for q in range(4):
            add(part, (core, q // 2, q % 2), r0[q // 2, q % 2])
        rs[b, 1] = send(part.at[core, :, 1 - xx, pl.ds(0, h)], r1a, rssem, (b, 1), at_tp(2))
        rs[b, 2] = send(part.at[core, 1 - yy, :, pl.ds(h, h)], r1b, rssem, (b, 2), at_tp(4))

    def rs2(b):
        part, r0, r1a, r1b, r2a, r2b = rs_refs(b)
        h = part.shape[3] // 2
        rs[b, 1].wait_recv()
        add(part, (core, 1 - yy, xx, pl.ds(0, h)), r1a[1 - yy])
        rs[b, 3] = send(part.at[core, 1 - yy, xx, pl.ds(0, h)], r2a, rssem, (b, 3), at_tp(4))
        rs[b, 2].wait_recv()
        add(part, (core, yy, 1 - xx, pl.ds(h, h)), r1b[1 - xx])
        rs[b, 4] = send(part.at[core, yy, 1 - xx, pl.ds(h, h)], r2b, rssem, (b, 4), at_tp(2))

    def rs3(b):
        part, r0, r1a, r1b, r2a, r2b = rs_refs(b)
        h = part.shape[3] // 2
        rs[b, 3].wait_recv()
        upper = part[core, yy, xx, pl.ds(0, h)].astype(F32) + r1a[yy].astype(F32) + r2a[...].astype(F32)
        if b == 0:
            total[pl.ds(0, h), :] = upper
        else:
            fin[b - 1, pl.ds(0, h), :] = upper.astype(BF)
        rs[b, 4].wait_recv()
        lower = part[core, yy, xx, pl.ds(h, h)].astype(F32) + r1b[xx].astype(F32) + r2b[...].astype(F32)
        if b == 0:
            total[pl.ds(h, h), :] = lower
        else:
            fin[b - 1, pl.ds(h, h), :] = lower.astype(BF)
            back = lax.rem(me + experts - b, experts)
            rs[b, 5] = send(fin.at[b - 1], ret.at[b - 1], retsem, (b - 1,), (back, tp))

    def partials(b):
        part = rs_refs(b)[0]

        def one(which):
            def body(q, carry):
                at = span(2 * q + which)
                value = jnp.dot(hid[...], dw[:, at], preferred_element_type=F32)
                part[which, q // 2, q % 2] = value.astype(BF)
                return carry

            lax.fori_loop(0, 4, body, 0)

        one(1 - core)
        rs0(b)
        one(core)

    def dense_partials():
        pair = combine(me)

        def one(which):
            def body(q, carry):
                k = 2 * q + which
                at = span(k)
                value = jnp.dot(hid[...], dw[:, at], preferred_element_type=F32).astype(BF)
                side = jnp.dot(dhid[...], dd[:, at], preferred_element_type=F32)
                part_l[which, q // 2, q % 2] = (
                    mix(pair, value) + jax.nn.sigmoid(gates[k]) * side
                ).astype(BF)
                return carry

            lax.fori_loop(0, 4, body, 0)

        one(1 - core)
        rs0(0)
        one(core)

    def returned(b):
        rs[b, 5].wait_recv()
        total[...] += mix(combine(ring(b)), ret[b - 1])

    first, second, third = order
    ag1(first)
    loads[0].wait()
    loads[1].wait()
    hidden(xloc)
    ag1(second)
    loads[2].wait()
    loads[3].wait()
    acts = jnp.dot(normed[...], dgu[...], preferred_element_type=F32)
    dhid[...] = silu_mul(acts[:, :dsp], acts[:, dsp:])
    ag1(third)
    ag2(first)
    loads[4].wait()
    loads[5].wait()
    for copy in gcopies:
        copy.wait_recv()
    dense_partials()
    ag2(second)
    ag3(first)
    rs1(0)
    ag_done(first)
    hidden(xbuf.at[first - 1])
    ag2(third)
    ag3(second)
    partials(first)
    rs2(0)
    ag3(third)
    rs1(first)
    ag_done(second)
    hidden(xbuf.at[second - 1])
    rs3(0)
    partials(second)
    rs2(first)
    rs1(second)
    ag_done(third)
    hidden(xbuf.at[third - 1])
    rs3(first)
    partials(third)
    rs2(second)
    rs1(third)
    rs3(second)
    returned(first)
    rs2(third)
    returned(second)
    rs3(third)
    returned(third)
    out_ref[...] = total[...].astype(BF)
    for copy in pending:
        copy.wait_send()


def fused_local(
    tokens,
    norm_gain,
    expert_ids,
    routing_weight,
    expert_gate,
    expert_up,
    expert_down,
    dense_gate_w,
    dense_up_w,
    dense_down_w,
    dense_gate,
):
    experts = lax.axis_size("ep")
    parts = lax.axis_size("tp")
    group, width = tokens.shape
    cap = 3 * group // experts
    cols = width // parts
    ffp = expert_gate.shape[2]
    dsp = dense_gate_w.shape[1]
    rounds = experts - 1
    vmem, hbm = pl.BlockSpec(memory_space=pltpu.VMEM), pl.BlockSpec(memory_space=pl.ANY)
    dma = pltpu.SemaphoreType.DMA
    half, ghalf = cap // 2, group // 2
    return pl.pallas_call(
        functools.partial(fused_kernel, experts),
        out_shape=jax.ShapeDtypeStruct((group, cols), BF),
        in_specs=[vmem] * 4 + [hbm] * 6 + [vmem],
        out_specs=vmem,
        scratch_shapes=[
            pltpu.VMEM((width, ffp), BF),
            pltpu.VMEM((width, ffp), BF),
            pltpu.VMEM((ffp, width), BF),
            pltpu.VMEM((width, 2 * dsp), BF),
            pltpu.VMEM((dsp, width), BF),
            pltpu.VMEM((group, width), BF),
            pltpu.VMEM((128, group), F32),
            pltpu.VMEM((group, 128), F32),
            pltpu.VMEM((parts, 1, cols), F32),
            pltpu.VMEM((rounds, cap, cols), BF),
            pltpu.VMEM((cap, width), BF),
            pltpu.VMEM((rounds, cap, width), BF),
            pltpu.VMEM((cap, ffp), BF),
            pltpu.VMEM((group, dsp), BF),
            pltpu.VMEM((2, 2, 2, group, cols), BF),
            pltpu.VMEM((rounds, 2, 2, 2, cap, cols), BF),
            pltpu.VMEM((2, 2, group, cols), BF),
            pltpu.VMEM((rounds, 2, 2, cap, cols), BF),
            pltpu.VMEM((2, ghalf, cols), BF),
            pltpu.VMEM((2, ghalf, cols), BF),
            pltpu.VMEM((rounds, 2, half, cols), BF),
            pltpu.VMEM((rounds, 2, half, cols), BF),
            pltpu.VMEM((ghalf, cols), BF),
            pltpu.VMEM((ghalf, cols), BF),
            pltpu.VMEM((rounds, half, cols), BF),
            pltpu.VMEM((rounds, half, cols), BF),
            pltpu.VMEM((rounds, cap, cols), BF),
            pltpu.VMEM((rounds, cap, cols), BF),
            pltpu.VMEM((group, cols), F32),
            dma((6,)),
            dma((2, parts - 1)),
            dma((2, rounds)),
            dma((2, rounds, 9)),
            dma((2, experts, 5)),
            dma((2, rounds)),
        ],
        compiler_params=pltpu.CompilerParams(
            collective_id=0, has_side_effects=True, vmem_limit_bytes=56 * 1024 * 1024
        ),
        name="routed_layer",
    )(
        tokens,
        norm_gain[None, :],
        expert_ids,
        routing_weight,
        expert_gate,
        expert_up,
        expert_down,
        dense_gate_w,
        dense_up_w,
        dense_down_w,
        dense_gate[None, :],
    )


def local(*args):
    experts, parts = lax.axis_size("ep"), lax.axis_size("tp")
    group, width = args[0].shape
    fits = (
        experts == 4
        and parts == 8
        and width % (128 * parts) == 0
        and group % 128 == 0
        and (3 * group // experts) % 32 == 0
        and args[7].shape[1] % 128 == 0
        and args[4].shape[2] % 16 == 0
    )
    return (fused_local if fits else plain_local)(*args)


def solution(mesh):
    return jax.shard_map(
        local,
        mesh=mesh,
        in_specs=(
            P("ep", None),
            P(),
            P("ep", None),
            P("ep", None),
            P("ep", None, "tp"),
            P("ep", None, "tp"),
            P("ep", "tp", None),
            P(None, "tp"),
            P(None, "tp"),
            P("tp", None),
            P("tp"),
        ),
        out_specs=P("ep", "tp"),
        check_vma=False,
    )
```

```python
import functools
import jax
import jax.numpy as jnp
from jax import lax
from jax.experimental import pallas as pl
from jax.experimental.pallas import tpu as pltpu
from jax.sharding import PartitionSpec as P

EPSILON = 1e-06


def positions(block_ids, experts, capacity):
    flat_ids = block_ids.reshape(-1)
    one_hot = (flat_ids[:, None] == jnp.arange(experts, dtype=jnp.int32)[None, :]).astype(jnp.int32)
    earlier = jnp.cumsum(one_hot, axis=0) - one_hot
    return flat_ids * capacity + jnp.sum(earlier * one_hot, axis=1)


def transposed_term(hidden, down_w):
    return lax.dot_general(
        down_w, hidden, (((0,), (1,)), ((), ())), preferred_element_type=jnp.float32
    )


def plain_local(
    tokens,
    norm_gain,
    expert_ids,
    routing_weight,
    expert_gate,
    expert_up,
    expert_down,
    dense_gate_w,
    dense_up_w,
    dense_down_w,
    dense_gate,
):
    experts = lax.axis_size("ep")
    group_tokens, model_width = tokens.shape
    capacity = 3 * group_tokens // experts
    slots_all = experts * capacity
    part_rows = model_width // lax.axis_size("tp")
    values = tokens.astype(jnp.float32)
    factor = lax.rsqrt(jnp.mean(values * values, axis=-1, keepdims=True) + EPSILON)
    normed = (values * factor * norm_gain[None, :]).astype(jnp.bfloat16)
    places = positions(expert_ids, experts, capacity)
    token_no = jnp.arange(2 * group_tokens, dtype=jnp.int32) // 2 + 1
    sources = jnp.zeros((slots_all,), jnp.int32).at[places].set(token_no)
    padded = jnp.concatenate([jnp.zeros((1, model_width), jnp.bfloat16), normed], axis=0)
    gate_w = expert_gate[0]
    up_w = expert_up[0]
    down_w = expert_down[0]
    first_col = lax.axis_index("tp") * part_rows
    column_part = lax.dynamic_slice_in_dim(padded, first_col, part_rows, 1)
    outgoing = column_part[sources].reshape(experts, capacity, part_rows)
    landed = lax.all_to_all(outgoing, "ep", split_axis=0, concat_axis=0, tiled=True)
    portion = lax.all_gather(landed, "tp", axis=2, tiled=True)
    columns = portion.reshape(slots_all, portion.shape[2])
    gate_act = jnp.dot(columns, gate_w, preferred_element_type=jnp.float32)
    up_act = jnp.dot(columns, up_w, preferred_element_type=jnp.float32)
    hidden = (jax.nn.silu(gate_act) * up_act).astype(jnp.bfloat16)
    dense_gate_act = jnp.dot(normed, dense_gate_w, preferred_element_type=jnp.float32)
    dense_up_act = jnp.dot(normed, dense_up_w, preferred_element_type=jnp.float32)
    dense_hidden = (jax.nn.silu(dense_gate_act) * dense_up_act).astype(jnp.bfloat16)
    dense_out = lax.psum_scatter(
        transposed_term(dense_hidden, dense_down_w).astype(jnp.bfloat16),
        "tp",
        scatter_dimension=0,
        tiled=True,
    ).astype(jnp.float32)
    expert_out = lax.psum_scatter(
        transposed_term(hidden, down_w).astype(jnp.bfloat16), "tp", scatter_dimension=0, tiled=True
    )
    expert_half = expert_out.reshape(part_rows, experts, capacity)
    returned = lax.all_to_all(expert_half, "ep", split_axis=1, concat_axis=1, tiled=True).reshape(
        part_rows, slots_all
    )
    picked = (
        jnp.take(returned, places, axis=1).astype(jnp.float32).reshape(part_rows, group_tokens, 2)
    )
    routed = jnp.sum(picked * routing_weight[None, :, :], axis=2)
    gate_factor = jax.nn.sigmoid(dense_gate)[:, None]
    return (routed + gate_factor * dense_out).T.astype(jnp.bfloat16)


BF = jnp.bfloat16
F32 = jnp.float32


def silu_mul(gate_act, up_act):
    return (gate_act / (1.0 + jnp.exp(-gate_act)) * up_act).astype(BF)


def dot_t(rows, weights):
    return lax.dot_general(rows, weights, (((1,), (1,)), ((), ())), preferred_element_type=F32)


def fused_kernel(
    experts,
    tok_ref,
    gain_ref,
    ids_ref,
    rw_ref,
    gw_hbm,
    uw_hbm,
    dw_hbm,
    dg_hbm,
    du_hbm,
    dd_hbm,
    dgate_ref,
    out_ref,
    gw,
    uw,
    dw,
    dgu,
    dd,
    normed,
    slot_row,
    slot_col,
    weight_col,
    gates,
    zsend,
    xloc,
    xbuf,
    hid,
    dhid,
    part_l,
    part_c,
    r0_l,
    r0_c,
    r1a_l,
    r1b_l,
    r1a_c,
    r1b_c,
    r2a_l,
    r2b_l,
    r2a_c,
    r2b_c,
    fin,
    ret,
    total,
    wsem,
    gsem,
    zsem,
    agsem,
    rssem,
    retsem,
):
    me = lax.axis_index("ep")
    tp = lax.axis_index("tp")
    core, xx, yy = tp % 2, (tp // 2) % 2, tp // 4
    group, width = tok_ref.shape
    cols = out_ref.shape[1]
    cap = zsend.shape[1]
    ffp = gw.shape[0]
    dsp = dd.shape[0]
    rounds = experts - 1
    mesh_id = pl.DeviceIdType.MESH

    def peer(flip):
        bits = (core + flip % 2) % 2, (xx + flip // 2 % 2) % 2, (yy + flip // 4) % 2
        return bits[2] * 4 + bits[1] * 2 + bits[0]

    def ring(d):
        return lax.rem(me + d, experts)

    barrier = pltpu.get_barrier_semaphore()
    for flip in range(1, 8):
        pl.semaphore_signal(barrier, 1, device_id=(me, peer(flip)), device_id_type=mesh_id)
    for d in range(1, experts):
        pl.semaphore_signal(barrier, 1, device_id=(ring(d), tp), device_id_type=mesh_id)

    loads = [
        pltpu.make_async_copy(gw_hbm.at[0], gw, wsem.at[0]),
        pltpu.make_async_copy(uw_hbm.at[0], uw, wsem.at[1]),
        pltpu.make_async_copy(dg_hbm, dgu.at[:, pl.ds(0, dsp)], wsem.at[2]),
        pltpu.make_async_copy(du_hbm, dgu.at[:, pl.ds(dsp, dsp)], wsem.at[3]),
        pltpu.make_async_copy(dw_hbm.at[0], dw, wsem.at[4]),
        pltpu.make_async_copy(dd_hbm, dd, wsem.at[5]),
    ]
    for load in loads:
        load.start()

    gain = gain_ref[...]
    step = 32

    def norm_rows(i, carry):
        rows = pl.ds(pl.multiple_of(i * step, step), step)
        values = tok_ref[rows, :].astype(F32)
        factor = lax.rsqrt(jnp.sum(values * values, axis=1, keepdims=True) * (1.0 / width) + EPSILON)
        normed[rows, :] = (values * factor * gain).astype(BF)
        return carry

    lax.fori_loop(0, group // step, norm_rows, 0)

    id0, id1 = ids_ref[0:1, :], ids_ref[1:2, :]
    number = lax.broadcasted_iota(jnp.int32, (128, group), 0)
    named = (id0 == number) | (id1 == number)
    earlier = jnp.where(
        lax.broadcasted_iota(jnp.int32, (group, group), 0)
        < lax.broadcasted_iota(jnp.int32, (group, group), 1),
        1.0,
        0.0,
    ).astype(BF)
    marks = jnp.where(named, 1.0, 0.0).astype(BF)
    count = jnp.dot(marks, earlier, preferred_element_type=F32)
    slots = jnp.where(named, count, -1.0)
    weights = jnp.where(id0 == number, rw_ref[0:1, :], 0.0) + jnp.where(id1 == number, rw_ref[1:2, :], 0.0)
    slot_row[...] = slots
    slot_col[...] = slots.T
    weight_col[...] = weights.T
    lane = lax.broadcasted_iota(jnp.int32, (group, 128), 1)

    def pick(e):
        row = slot_row[pl.ds(e, 1), :].astype(jnp.int32)
        where = lax.broadcasted_iota(jnp.int32, (cap, group), 0)
        return jnp.where(row == where, 1.0, 0.0).astype(BF)

    def combine(e):
        slot = jnp.sum(jnp.where(lane == e, slot_col[...], 0.0), axis=1, keepdims=True).astype(jnp.int32)
        weight = jnp.sum(jnp.where(lane == e, weight_col[...], 0.0), axis=1, keepdims=True)
        where = lax.broadcasted_iota(jnp.int32, (group, cap), 1)
        full = jnp.where(slot == where, weight, 0.0)
        high = full.astype(BF)
        return high, (full - high.astype(F32)).astype(BF)

    def mix(pair, rows):
        return jnp.dot(pair[0], rows, preferred_element_type=F32) + jnp.dot(
            pair[1], rows, preferred_element_type=F32
        )

    pl.semaphore_wait(barrier, 7 + rounds)

    pending = []

    def send(src, dst, sems, index, target):
        copy = pltpu.make_async_remote_copy(
            src_ref=src,
            dst_ref=dst,
            send_sem=sems.at[(0,) + index],
            recv_sem=sems.at[(1,) + index],
            device_id=target,
            device_id_type=mesh_id,
        )
        copy.start()
        pending.append(copy)
        return copy

    def at_tp(flip):
        return (me, peer(flip))

    def span(slice_no):
        return pl.ds(pl.multiple_of(slice_no * cols, cols), cols)

    zcopies, order = {}, list(range(1, experts))
    if rounds == 3:
        order = [1, 3, 2]
    for d in order:
        rows = jnp.dot(pick(ring(d)), normed[:, span(tp)], preferred_element_type=F32)
        zsend[d - 1] = rows.astype(BF)
        zcopies[d] = send(zsend.at[d - 1], xbuf.at[d - 1, :, span(tp)], zsem, (d - 1,), (ring(d), tp))
    gcopies = [send(dgate_ref, gates.at[tp], gsem, (f - 1,), at_tp(f)) for f in range(1, 8)]
    gates[tp] = dgate_ref[...]
    here = pick(me)

    def local_rows(k, carry):
        at = pl.ds(pl.multiple_of(k * cols, cols), cols)
        xloc[:, at] = jnp.dot(here, normed[:, at], preferred_element_type=F32).astype(BF)
        return carry

    lax.fori_loop(0, width // cols, local_rows, 0)

    half = cap // 2
    top, bottom = pl.ds(0, half), pl.ds(half, half)
    everything = pl.ds(0, cap)
    ag = {}

    def move(d, name, number, rows, slice_flip, flip):
        ref = xbuf.at[d - 1, rows, span(peer(slice_flip))]
        ag[d, name] = send(ref, ref, agsem, (d - 1, number), at_tp(flip))

    def ag1(d):
        zcopies[d].wait_recv()
        move(d, "x", 0, everything, 0, 2)
        move(d, "y", 1, everything, 0, 4)
        move(d, "c", 2, everything, 0, 1)

    def ag2(d):
        ag[d, "x"].wait_recv()
        move(d, "xy", 3, top, 2, 4)
        move(d, "xc", 4, everything, 2, 1)
        ag[d, "y"].wait_recv()
        move(d, "yx", 5, bottom, 4, 2)
        move(d, "yc", 6, everything, 4, 1)

    def ag3(d):
        ag[d, "xy"].wait_recv()
        move(d, "xyc", 7, top, 6, 1)
        ag[d, "yx"].wait_recv()
        move(d, "yxc", 8, bottom, 6, 1)

    def ag_done(d):
        for name in ("c", "xc", "yc", "xyc", "yxc"):
            ag[d, name].wait_recv()

    tiles = [(n, min(256, ffp - n)) for n in range(0, ffp, 256)]

    def hidden(rows_ref):
        for n, size in tiles:
            gate_act = dot_t(rows_ref[...], gw[n : n + size, :])
            up_act = dot_t(rows_ref[...], uw[n : n + size, :])
            hid[:, n : n + size] = silu_mul(gate_act, up_act)

    def rs_refs(b):
        if b == 0:
            return part_l, r0_l, r1a_l, r1b_l, r2a_l, r2b_l
        return tuple(r.at[b - 1] for r in (part_c, r0_c, r1a_c, r1b_c, r2a_c, r2b_c))

    rs = {}

    def rs0(b):
        part, r0 = rs_refs(b)[:2]
        rs[b, 0] = send(part.at[1 - core], r0, rssem, (b, 0), at_tp(1))

    def add(dst, index, other):
        dst[index] = (dst[index].astype(F32) + other.astype(F32)).astype(BF)

    def rs1(b):
        part, r0, r1a, r1b = rs_refs(b)[:4]
        h = part.shape[3] // 2
        rs[b, 0].wait_recv()
        for q in range(4):
            add(part, (core, q // 2, q % 2), r0[q // 2, q % 2])
        rs[b, 1] = send(part.at[core, :, 1 - xx, pl.ds(0, h)], r1a, rssem, (b, 1), at_tp(2))
        rs[b, 2] = send(part.at[core, 1 - yy, :, pl.ds(h, h)], r1b, rssem, (b, 2), at_tp(4))

    def rs2(b):
        part, r0, r1a, r1b, r2a, r2b = rs_refs(b)
        h = part.shape[3] // 2
        rs[b, 1].wait_recv()
        add(part, (core, 1 - yy, xx, pl.ds(0, h)), r1a[1 - yy])
        rs[b, 3] = send(part.at[core, 1 - yy, xx, pl.ds(0, h)], r2a, rssem, (b, 3), at_tp(4))
        rs[b, 2].wait_recv()
        add(part, (core, yy, 1 - xx, pl.ds(h, h)), r1b[1 - xx])
        rs[b, 4] = send(part.at[core, yy, 1 - xx, pl.ds(h, h)], r2b, rssem, (b, 4), at_tp(2))

    def rs3(b):
        part, r0, r1a, r1b, r2a, r2b = rs_refs(b)
        h = part.shape[3] // 2
        rs[b, 3].wait_recv()
        upper = part[core, yy, xx, pl.ds(0, h)].astype(F32) + r1a[yy].astype(F32) + r2a[...].astype(F32)
        if b == 0:
            total[pl.ds(0, h), :] = upper
        else:
            fin[b - 1, pl.ds(0, h), :] = upper.astype(BF)
        rs[b, 4].wait_recv()
        lower = part[core, yy, xx, pl.ds(h, h)].astype(F32) + r1b[xx].astype(F32) + r2b[...].astype(F32)
        if b == 0:
            total[pl.ds(h, h), :] = lower
        else:
            fin[b - 1, pl.ds(h, h), :] = lower.astype(BF)
            back = lax.rem(me + experts - b, experts)
            rs[b, 5] = send(fin.at[b - 1], ret.at[b - 1], retsem, (b - 1,), (back, tp))

    def partials(b):
        part = rs_refs(b)[0]

        def one(which):
            def body(q, carry):
                at = span(2 * q + which)
                value = jnp.dot(hid[...], dw[:, at], preferred_element_type=F32)
                part[which, q // 2, q % 2] = value.astype(BF)
                return carry

            lax.fori_loop(0, 4, body, 0)

        one(1 - core)
        rs0(b)
        one(core)

    def dense_partials():
        pair = combine(me)

        def one(which):
            def body(q, carry):
                k = 2 * q + which
                at = span(k)
                value = jnp.dot(hid[...], dw[:, at], preferred_element_type=F32).astype(BF)
                side = jnp.dot(dhid[...], dd[:, at], preferred_element_type=F32)
                part_l[which, q // 2, q % 2] = (
                    mix(pair, value) + jax.nn.sigmoid(gates[k]) * side
                ).astype(BF)
                return carry

            lax.fori_loop(0, 4, body, 0)

        one(1 - core)
        rs0(0)
        one(core)

    def returned(b):
        rs[b, 5].wait_recv()
        total[...] += mix(combine(ring(b)), ret[b - 1])

    first, second, third = order
    loads[0].wait()
    loads[1].wait()
    hidden(xloc)
    ag1(first)
    loads[2].wait()
    loads[3].wait()
    acts = jnp.dot(normed[...], dgu[...], preferred_element_type=F32)
    dhid[...] = silu_mul(acts[:, :dsp], acts[:, dsp:])
    ag1(second)
    loads[4].wait()
    loads[5].wait()
    for copy in gcopies:
        copy.wait_recv()
    dense_partials()
    ag2(first)
    ag1(third)
    ag2(second)
    ag3(first)
    rs1(0)
    ag2(third)
    ag3(second)
    ag_done(first)
    hidden(xbuf.at[first - 1])
    partials(first)
    ag3(third)
    rs2(0)
    rs1(first)
    ag_done(second)
    hidden(xbuf.at[second - 1])
    partials(second)
    rs2(first)
    rs1(second)
    ag_done(third)
    hidden(xbuf.at[third - 1])
    partials(third)
    rs3(first)
    rs2(second)
    rs1(third)
    rs3(0)
    rs3(second)
    rs2(third)
    returned(first)
    returned(second)
    rs3(third)
    returned(third)
    out_ref[...] = total[...].astype(BF)
    for copy in pending:
        copy.wait_send()


def fused_local(
    tokens,
    norm_gain,
    expert_ids,
    routing_weight,
    expert_gate,
    expert_up,
    expert_down,
    dense_gate_w,
    dense_up_w,
    dense_down_w,
    dense_gate,
):
    experts = lax.axis_size("ep")
    parts = lax.axis_size("tp")
    group, width = tokens.shape
    cap = 3 * group // experts
    cols = width // parts
    ffp = expert_gate.shape[2]
    dsp = dense_gate_w.shape[1]
    rounds = experts - 1
    vmem, hbm = pl.BlockSpec(memory_space=pltpu.VMEM), pl.BlockSpec(memory_space=pl.ANY)
    dma = pltpu.SemaphoreType.DMA
    half, ghalf = cap // 2, group // 2
    return pl.pallas_call(
        functools.partial(fused_kernel, experts),
        out_shape=jax.ShapeDtypeStruct((group, cols), BF),
        in_specs=[vmem] * 4 + [hbm] * 6 + [vmem],
        out_specs=vmem,
        scratch_shapes=[
            pltpu.VMEM((ffp, width), BF),
            pltpu.VMEM((ffp, width), BF),
            pltpu.VMEM((ffp, width), BF),
            pltpu.VMEM((width, 2 * dsp), BF),
            pltpu.VMEM((dsp, width), BF),
            pltpu.VMEM((group, width), BF),
            pltpu.VMEM((128, group), F32),
            pltpu.VMEM((group, 128), F32),
            pltpu.VMEM((group, 128), F32),
            pltpu.VMEM((parts, 1, cols), F32),
            pltpu.VMEM((rounds, cap, cols), BF),
            pltpu.VMEM((cap, width), BF),
            pltpu.VMEM((rounds, cap, width), BF),
            pltpu.VMEM((cap, ffp), BF),
            pltpu.VMEM((group, dsp), BF),
            pltpu.VMEM((2, 2, 2, group, cols), BF),
            pltpu.VMEM((rounds, 2, 2, 2, cap, cols), BF),
            pltpu.VMEM((2, 2, group, cols), BF),
            pltpu.VMEM((rounds, 2, 2, cap, cols), BF),
            pltpu.VMEM((2, ghalf, cols), BF),
            pltpu.VMEM((2, ghalf, cols), BF),
            pltpu.VMEM((rounds, 2, half, cols), BF),
            pltpu.VMEM((rounds, 2, half, cols), BF),
            pltpu.VMEM((ghalf, cols), BF),
            pltpu.VMEM((ghalf, cols), BF),
            pltpu.VMEM((rounds, half, cols), BF),
            pltpu.VMEM((rounds, half, cols), BF),
            pltpu.VMEM((rounds, cap, cols), BF),
            pltpu.VMEM((rounds, cap, cols), BF),
            pltpu.VMEM((group, cols), F32),
            dma((6,)),
            dma((2, parts - 1)),
            dma((2, rounds)),
            dma((2, rounds, 9)),
            dma((2, experts, 5)),
            dma((2, rounds)),
        ],
        compiler_params=pltpu.CompilerParams(
            collective_id=0, has_side_effects=True, vmem_limit_bytes=56 * 1024 * 1024
        ),
        name="routed_layer",
    )(
        tokens,
        norm_gain[None, :],
        expert_ids.T,
        routing_weight.T,
        jnp.swapaxes(expert_gate, 1, 2),
        jnp.swapaxes(expert_up, 1, 2),
        expert_down,
        dense_gate_w,
        dense_up_w,
        dense_down_w,
        dense_gate[None, :],
    )


def local(*args):
    experts, parts = lax.axis_size("ep"), lax.axis_size("tp")
    group, width = args[0].shape
    fits = (
        experts == 4
        and parts == 8
        and width % (128 * parts) == 0
        and group % 128 == 0
        and (3 * group // experts) % 32 == 0
        and args[7].shape[1] % 128 == 0
        and args[4].shape[2] % 16 == 0
    )
    return (fused_local if fits else plain_local)(*args)


def solution(mesh):
    return jax.shard_map(
        local,
        mesh=mesh,
        in_specs=(
            P("ep", None),
            P(),
            P("ep", None),
            P("ep", None),
            P("ep", None, "tp"),
            P("ep", None, "tp"),
            P("ep", "tp", None),
            P(None, "tp"),
            P(None, "tp"),
            P("tp", None),
            P("tp"),
        ),
        out_specs=P("ep", "tp"),
        check_vma=False,
    )
```
